32 devices in a mesh: sp: 8 (over z, y), tp: 4 (over x, core).
Axes of the slice: x: 2, y: 2, z: 4, core: 2. Of those that a mesh axis runs over, the one named last changes fastest.
Arguments:
- resid: bfloat16 [4096, 2048], P(('sp', 'tp')), may hold values from -6 to 6
- query: bfloat16 [4096, 2048], P('sp', 'tp'), may hold values from -6 to 6
- forget_logits: bfloat16 [4096, 2048], P('sp', 'tp'), may hold values from -5 to 5
- forget_margin: float32 [2048], P('tp'), may hold values from 0 to 0.07, as said below
- decay_spike: float32 [4096, 16], P('sp', 'tp'), may hold values from -0.75 to 0
- value_logits: bfloat16 [4096, 2048], P('sp', 'tp'), may hold values from -6 to 6
- output_gate_logits: bfloat16 [4096, 2048], P('sp', 'tp'), may hold values from -6 to 6
- head_norm_scale: float32 [2048], P('tp'), may hold values from 0.1 to 1.9
- output_matrix: bfloat16 [2048, 2048], replicated, may hold values from -0.125 to 0.125
- norm_scale_vector: float32 [2048], replicated, may hold values from 0.1 to 1.9
- routes: int32 [4096, 2], P(('sp', 'tp')), may hold values from 0 to 31, all different within a row; in each aligned block of 128 rows (0 to 127, 128 to 255, ...) at most 16 rows name the same one
- routing_weight: float32 [4096, 2], P(('sp', 'tp')), may hold values from 0.2 to 1
- gate_matrix: bfloat16 [32, 2048, 1024], P(('sp', 'tp')), may hold values from -0.125 to 0.125
- up_matrix: bfloat16 [32, 2048, 1024], P(('sp', 'tp')), may hold values from -0.125 to 0.125
- down_matrix: bfloat16 [32, 1024, 2048], P(('sp', 'tp')), may hold values from -0.1875 to 0.1875
Outputs:
- result: bfloat16 [4096, 2048], P(('sp', 'tp'))
The draws below stay inside these ranges and needn't reach their ends.
Inputs may be any that keep to these rules, and one draw needn't show every extreme that they name: `routes`: within the rows of one device no expert is named by more than 16 rows; some device names some expert exactly 16 times in every draw. `forget_margin`: Positive.
All inputs are finite; a program needn't handle non-finite values.
Results may differ from the reference program's by a relative error of at most 0.012.
Values may be sent and summed in bfloat16 or wider, within the bound.
A program may use at most 128 MiB of HBM per device.

```python
import math
import jax
import jax.numpy as jnp
import numpy as np
from jax import lax

D = 2048
HEAD_TOTAL = 16
DK = 128
DV = 128
FF = 1024
TOP = 2
BLOCK = 64
TOKENS_PER_SHARD = 512
SEQUENCE_TOKENS = 4096
ROWS = 128
EXPERTS = 32
CAP = 16
DEVICES = 32


def slow_choice(key):
    pick_key, slow_key, fast_key = jax.random.split(jax.random.fold_in(key, 11), 3)
    ranking = jax.random.permutation(pick_key, HEAD_TOTAL)
    slow_heads = ranking < HEAD_TOTAL // 2
    return (slow_heads, slow_key, fast_key)


def draw_forget_margin(key, part):
    slow_heads, slow_key, fast_key = slow_choice(key)
    slow_gap = jnp.exp(jax.random.uniform(slow_key, (HEAD_TOTAL, DK), jnp.float32, jnp.log(0.3), jnp.log(1.5))) / SEQUENCE_TOKENS
    fast_gap = jnp.exp(jax.random.uniform(fast_key, (HEAD_TOTAL, DK), jnp.float32, jnp.log(0.02), jnp.log(0.066)))
    return jnp.where(slow_heads[:, None], slow_gap, fast_gap).reshape(HEAD_TOTAL * DK)


def draw_forget_logits(key, part):
    jitter_key, shift_key = jax.random.split(jax.random.fold_in(key, 23))
    block_count = SEQUENCE_TOKENS // TOKENS_PER_SHARD
    shifts = jax.random.uniform(shift_key, (block_count, HEAD_TOTAL), jnp.float32, -1.0, 1.0)
    jitter = jnp.clip(jax.random.normal(jitter_key, (SEQUENCE_TOKENS, HEAD_TOTAL * DK), jnp.float32), -4.0, 4.0)
    block_shift = jnp.repeat(jnp.repeat(shifts, TOKENS_PER_SHARD, axis=0), DK, axis=1)
    return (jitter + block_shift).astype(jnp.bfloat16)


def draw_decay_spike(key, part):
    slow_heads, slow_key, fast_key = slow_choice(key)
    position_seed, spike_size_seed, rate_seed = jax.random.split(jax.random.fold_in(key, 37), 3)
    spike_positions = jax.random.randint(position_seed, (3, HEAD_TOTAL), 0, SEQUENCE_TOKENS)
    spike_magnitudes = jnp.log(jax.random.uniform(spike_size_seed, (3, HEAD_TOTAL), jnp.float32, 0.5, 0.8))
    position_entries = jnp.arange(SEQUENCE_TOKENS, dtype=jnp.int32)[:, None, None] == spike_positions[None, :, :]
    spike_events = jnp.sum(jnp.where(position_entries, spike_magnitudes[None, :, :], 0.0), axis=1)
    block_count = SEQUENCE_TOKENS // TOKENS_PER_SHARD
    additional_rate = -jax.random.uniform(rate_seed, (block_count, HEAD_TOTAL), jnp.float32, 0.005, 0.045)
    additional_rate = jnp.where(slow_heads[None, :], 0.0, additional_rate)
    return spike_events + jnp.repeat(additional_rate, TOKENS_PER_SHARD, axis=0)


def shard_levels(own_key, extent, pieces, low, top_value):
    gain = 1.0
    for axis_at, blocks in pieces:
        draws = jax.random.uniform(jax.random.fold_in(jax.random.fold_in(own_key, 6), axis_at), (blocks,), jnp.float32, low / len(pieces), top_value / len(pieces))
        gain = gain * jnp.repeat(jnp.exp(draws), extent[axis_at] // blocks).reshape((-1,) + (1,) * (len(extent) - 1 - axis_at))
    return gain


def shared_out(stream_key, own, number, rows, amount, top, reach, slope):
    order = jax.random.permutation(stream_key, amount)
    heavy_load, common = load_shares(amount, rows * top, reach, slope, True), load_shares(amount, rows * top, reach, slope, False)
    places = jnp.arange(amount)

    def named(sizes, offset_by):
        used = int((sizes > 0).sum())
        fixed = max(1, used // 4)
        passed = fixed + (places - fixed + offset_by * (used - fixed)) % max(1, amount - fixed)
        return jnp.zeros((amount,), jnp.int32).at[order[jnp.where(places < fixed, places, passed)]].set(jnp.asarray(sizes, jnp.int32))

    sizes = jnp.where(number % 4 == 0, named(heavy_load, number // 4), named(common, number - number // 4 - 1))
    mixed = jax.random.permutation(jax.random.fold_in(own, 3), amount)
    giver, taker = mixed[0:amount // 2 * 2:2], mixed[1:amount // 2 * 2:2]
    slack = jnp.minimum(sizes[giver] - 1, reach - sizes[taker]) // 2
    slack = jnp.where((giver == order[0]) | (taker == order[0]) | (sizes[taker] == 0), 0, jnp.maximum(slack, 0))
    passed = jax.random.randint(jax.random.fold_in(own, 4), (amount // 2,), 0, 1 << 20) % (slack + 1)
    sizes = sizes.at[giver].add(-passed).at[taker].add(passed)
    members = jnp.searchsorted(jnp.cumsum(sizes), jnp.arange(rows * top), side="right").astype(jnp.int32)
    grid = members.reshape(top, rows).T
    grid = grid[jax.random.permutation(jax.random.fold_in(own, 1), rows)]
    offset_by = jax.random.randint(jax.random.fold_in(own, 2), (rows, 1), 0, top)
    return jnp.take_along_axis(grid, (jnp.arange(top)[None, :] + offset_by) % top, axis=1)


def load_shares(amount, total, limit, slope, full):
    loads = [(1 << 20) // math.isqrt(standing ** slope) + 1 for standing in range(1, amount + 1)]
    largest = limit if full else min(limit, max(-(-total // amount), total * loads[0] // sum(loads)))
    least = 1 if total - largest >= amount - 1 else 0
    holding, spare = [largest] + [least] * (amount - 1), total - largest - least * (amount - 1)
    while spare > 0:
        movable = [i for i in range(1, amount) if holding[i] < largest] or [i for i in range(1, amount) if holding[i] < limit]
        whole, left = sum([loads[i] for i in movable]), spare
        for i in movable:
            extra = min(limit - holding[i], max(1, left * loads[i] // whole), spare)
            holding[i] = holding[i] + extra
            spare = spare - extra
    return np.array(holding)


def centred(key, dims, deviation, most, pieces=(), held_as=jnp.bfloat16):
    drawn = jax.random.normal(key, dims, jnp.float32) * deviation
    if len(pieces) > 0:
        drawn = shard_levels(key, dims, pieces, -0.22, 0.18) * drawn
    return jnp.clip(drawn, min=-most, max=most).astype(held_as)


def setup_inputs(seed: int = 0) -> dict:
    splits = jax.random.split(jax.random.key(seed), 16)
    resid = centred(splits[0], (SEQUENCE_TOKENS, D), 1.0, 6.0, ((0, 32),))
    query = centred(splits[1], (SEQUENCE_TOKENS, HEAD_TOTAL * DK), 1.0, 6.0, ((0, 8), (1, 4)))
    forget_logits = draw_forget_logits(jax.random.fold_in(splits[15], 71), 0)
    forget_margin = draw_forget_margin(jax.random.fold_in(splits[15], 71), 0)
    decay_spike = draw_decay_spike(jax.random.fold_in(splits[15], 71), 0)
    value_logits = centred(splits[5], (SEQUENCE_TOKENS, HEAD_TOTAL * DV), 1.0, 6.0, ((0, 8), (1, 4)))
    output_gate_logits = centred(splits[6], (SEQUENCE_TOKENS, HEAD_TOTAL * DV), 1.0, 6.0, ((0, 8), (1, 4)))
    head_norm_scale = jnp.clip(1.0 + 0.18 * jax.random.normal(splits[7], (HEAD_TOTAL * DV,), jnp.float32), 0.1, 1.9)
    output_matrix = centred(splits[8], (HEAD_TOTAL * DV, D), (HEAD_TOTAL * DV) ** -0.5, 0.125)
    norm_scale_vector = jnp.clip(1.0 + 0.18 * jax.random.normal(splits[9], (D,), jnp.float32), 0.1, 1.9)
    routes_keys = jax.random.split(jax.random.fold_in(splits[10], 1), SEQUENCE_TOKENS // ROWS)
    routes_turns = jax.random.permutation(jax.random.fold_in(splits[10], 3), SEQUENCE_TOKENS // ROWS)
    routes = jax.vmap(lambda own, number: shared_out(jax.random.fold_in(splits[10], 2), own, number, ROWS, EXPERTS, TOP, CAP, 2))(routes_keys, routes_turns).reshape((SEQUENCE_TOKENS, TOP))
    routing_weight = jnp.clip(0.2 + 0.8 * jax.random.uniform(splits[11], (SEQUENCE_TOKENS, TOP), jnp.float32) ** shard_levels(splits[11], (SEQUENCE_TOKENS, TOP), ((0, 32),), -0.2, 0.2), 0.2, 1.0)
    gate_matrix = centred(splits[12], (EXPERTS, D, FF), D ** -0.5, 0.125, ((0, 32),))
    up_matrix = centred(splits[13], (EXPERTS, D, FF), D ** -0.5, 0.125, ((0, 32),))
    down_matrix = centred(splits[14], (EXPERTS, FF, D), FF ** -0.5, 0.1875, ((0, 32),))
    return {"resid": resid, "query": query, "forget_logits": forget_logits, "forget_margin": forget_margin, "decay_spike": decay_spike, "value_logits": value_logits, "output_gate_logits": output_gate_logits, "head_norm_scale": head_norm_scale, "output_matrix": output_matrix, "norm_scale_vector": norm_scale_vector, "routes": routes, "routing_weight": routing_weight, "gate_matrix": gate_matrix, "up_matrix": up_matrix, "down_matrix": down_matrix}


maximum_value = lax.Precision.HIGHEST

def to_blocks(matrix, head_number):
    length, columns = matrix.shape
    return matrix.reshape(length // BLOCK, BLOCK, head_number, columns // head_number).transpose(0, 2, 1, 3)

def from_blocks(matrix):
    block_count, head_number, span_len, head_width = matrix.shape
    return matrix.transpose(0, 2, 1, 3).reshape(block_count * span_len, head_number * head_width)

def input_lookup(query, forget_logits, forget_margin, decay_spike, value_logits):
    head_number = decay_spike.shape[1]
    every_key = forget_margin[None, :] * jax.nn.sigmoid(-forget_logits.astype(jnp.float32))
    head_width = every_key.shape[1] // head_number
    logarithm_of_decay = jnp.log1p(-every_key) + jnp.repeat(decay_spike, head_width, axis=1)
    queries = query.astype(jnp.float32) * DK ** (-0.5)
    values = jax.nn.silu(value_logits.astype(jnp.float32))
    return (to_blocks(queries, head_number), to_blocks(every_key, head_number), to_blocks(values, head_number), to_blocks(logarithm_of_decay, head_number))

def block_recurrence(queries, keys_in, values, logarithm_of_decay):
    span_len = queries.shape[2]
    causal = (lax.broadcasted_iota(jnp.int32, (span_len, span_len), 0) >= lax.broadcasted_iota(jnp.int32, (span_len, span_len), 1))[:, :, None]
    cum_log = jnp.cumsum(logarithm_of_decay, axis=2)

    def advance(current_state, inputs):
        query_block, key_b, value_block, cumulative_block = inputs
        spread = cumulative_block[:, :, None, :] - cumulative_block[:, None, :, :]
        weight_t = jnp.where(causal, jnp.exp(jnp.where(causal, spread, 0.0)), 0.0)
        router_scores = jnp.einsum('htk,hsk,htsk->hts', query_block, key_b, weight_t, precision=maximum_value)
        within = jnp.einsum('hts,hsv->htv', router_scores, value_block, precision=maximum_value)
        incoming_state = jnp.einsum('bup,bpl->bul', query_block * jnp.exp(cumulative_block), current_state, precision=maximum_value)
        final_block = cumulative_block[:, -1, :]
        decayed_state = key_b * jnp.exp(final_block[:, None, :] - cumulative_block)
        following_state = jnp.exp(final_block)[:, :, None] * current_state + jnp.einsum('ixq,ixn->iqn', decayed_state, value_block, precision=maximum_value)
        return (following_state, within + incoming_state)
    start_state = jnp.zeros((queries.shape[1], queries.shape[3], values.shape[3]), jnp.float32)
    last_state, outputs = lax.scan(advance, start_state, (queries, keys_in, values, cum_log))
    return (last_state, outputs, cum_log)

def gate_rows(recurrence_output, output_gate_logits, head_norm_scale):
    square = lax.optimization_barrier(jnp.mean(recurrence_output * recurrence_output, axis=3, keepdims=True))
    scaled = from_blocks(recurrence_output * lax.rsqrt(square + 1e-06)) * head_norm_scale[None, :]
    return (scaled * jax.nn.silu(output_gate_logits.astype(jnp.float32))).astype(jnp.bfloat16)

def row_norm(stream, norm_scale_vector):
    values = stream.astype(jnp.float32)
    square = lax.optimization_barrier(jnp.mean(values * values, axis=1, keepdims=True))
    return (values * lax.rsqrt(square + 1e-06) * norm_scale_vector[None, :]).astype(jnp.bfloat16)

def reference(resid, query, forget_logits, forget_margin, decay_spike, value_logits, output_gate_logits, head_norm_scale, output_matrix, norm_scale_vector, routes, routing_weight, gate_matrix, up_matrix, down_matrix):
    block_list = input_lookup(query, forget_logits, forget_margin, decay_spike, value_logits)
    last_state, recurrence_output, cum_log = block_recurrence(*block_list)
    gated_rows = gate_rows(recurrence_output, output_gate_logits, head_norm_scale)
    mixed_rows = jnp.dot(gated_rows, output_matrix, preferred_element_type=jnp.float32)
    stream = (resid.astype(jnp.float32) + mixed_rows).astype(jnp.bfloat16)
    normed = row_norm(stream, norm_scale_vector)
    flat_routes = routes.reshape(-1)
    member = (flat_routes[:, None] == jnp.arange(EXPERTS, dtype=jnp.int32)[None, :]).astype(jnp.int32)
    slot_rank = lax.optimization_barrier(jnp.sum(jnp.cumsum(member, axis=0) * member, axis=1)) - 1
    slot_depth = DEVICES * CAP
    position_entries = (flat_routes * slot_depth + slot_rank).astype(jnp.int32)
    sources = (jnp.arange(flat_routes.shape[0], dtype=jnp.int32) // TOP).astype(jnp.int32)
    buffer = jnp.zeros((EXPERTS * slot_depth, D), jnp.bfloat16).at[position_entries].set(normed[sources])

    def expert_rows(inputs):
        slot_rows, gate_e, up_e, down_e = inputs
        gate_part = jnp.dot(slot_rows, gate_e, preferred_element_type=jnp.float32)
        up_part = jnp.dot(slot_rows, up_e, preferred_element_type=jnp.float32)
        hidden = (jax.nn.silu(gate_part) * up_part).astype(jnp.bfloat16)
        return jnp.dot(hidden, down_e, preferred_element_type=jnp.float32).astype(jnp.bfloat16)
    outputs = lax.map(expert_rows, (buffer.reshape(EXPERTS, slot_depth, D), gate_matrix, up_matrix, down_matrix))
    picked = outputs.reshape(EXPERTS * slot_depth, D)[position_entries].astype(jnp.float32).reshape(-1, TOP, D)
    combined = stream.astype(jnp.float32) + lax.optimization_barrier(jnp.sum(routing_weight[:, :, None] * picked, axis=1))
    return combined.astype(jnp.bfloat16)
```

```python
import jax
import jax.numpy as jnp
from jax import lax
from jax.experimental import pallas as pl
from jax.experimental.pallas import tpu as pltpu
from jax.sharding import PartitionSpec as P

DK = 128
BLOCK = 64


SPAN = 2 * BLOCK


def spread_dot(left, right, dims):
    return lax.dot_general(left, right, (dims, ((), ())), preferred_element_type=jnp.float32)


def mixing_kernel(
    q_ref, f_ref, m_ref, s_ref, v_ref, g_ref, n_ref, w_ref, r_ref, stream_ref,
    loc_ref, qt_ref, tot_ref, parts_ref, came_ref, answer_ref, back_ref, prior_ref, rows_ref,
    out_ref, matrix_ref,
    ready_sem, came_sem, answer_sem, back_sem, rows_sem, out_sem, matrix_sem,
):
    length, columns = q_ref.shape
    heads = s_ref.shape[0]
    width = columns // heads
    vwidth = v_ref.shape[1] // heads
    count, mates = lax.axis_size("sp"), lax.axis_size("tp")
    me, lane = lax.axis_index("sp"), lax.axis_index("tp")
    part = vwidth // count
    barrier = pltpu.get_barrier_semaphore()
    fetch = pltpu.make_async_copy(w_ref, matrix_ref, matrix_sem)
    fetch.start()
    for d in range(1, count):
        pl.semaphore_signal(
            barrier, inc=1, device_id={"sp": lax.rem(me + d, count)},
            device_id_type=pl.DeviceIdType.MESH,
        )
    for d in range(1, mates):
        pl.semaphore_signal(
            barrier, inc=1, device_id={"tp": lax.rem(lane + d, mates)},
            device_id_type=pl.DeviceIdType.MESH,
        )

    span = min(SPAN, length)
    lower = lax.broadcasted_iota(jnp.int32, (span, span), 0) >= lax.broadcasted_iota(
        jnp.int32, (span, span), 1
    )
    ones = lower.astype(jnp.float32).astype(jnp.bfloat16)
    spot = lax.broadcasted_iota(jnp.int32, (2 * heads, width), 0)

    def one_head(head, carry):
        here = pl.ds(pl.multiple_of(head * width, width), width)
        there = pl.ds(pl.multiple_of(head * vwidth, vwidth), vwidth)
        mine = ((spot == head) | (spot == head + heads)).astype(jnp.float32).astype(jnp.bfloat16)
        margin = m_ref[:, here]
        state = jnp.zeros((vwidth, width), jnp.float32)
        before = jnp.zeros((1, width), jnp.float32)
        for at in range(length // span):
            rows = pl.ds(at * span, span)
            keys = margin * jax.nn.sigmoid(-f_ref[rows, here].astype(jnp.float32))
            spikes = s_ref[:, rows]
            top = spikes.astype(jnp.bfloat16).astype(jnp.float32)
            halves = jnp.concatenate([top, spikes - top], axis=0).astype(jnp.bfloat16)
            decay = jnp.log1p(-keys) + spread_dot(halves, mine, ((0,), (0,)))
            high = decay.astype(jnp.bfloat16)
            low = (decay - high.astype(jnp.float32)).astype(jnp.bfloat16)
            both = spread_dot(ones, jnp.concatenate([high, low], axis=1), ((1,), (0,)))
            cum = both[:, :width] + both[:, width:]
            middle = cum[span // 2 - 1 : span // 2, :]
            last = cum[span - 1 : span, :]
            down = jnp.exp(cum - middle)
            up = jnp.exp(middle - cum)
            query = q_ref[rows, here].astype(jnp.float32) * DK ** (-0.5)
            logits = v_ref[rows, there].astype(jnp.float32)
            value = (logits * jax.nn.sigmoid(logits)).astype(jnp.bfloat16)
            near = query * down
            rise = keys * up
            score = spread_dot(
                near.astype(jnp.bfloat16), rise.astype(jnp.bfloat16), ((1,), (1,))
            )
            score = jnp.where(lower, score, 0.0).astype(jnp.bfloat16)
            result = spread_dot(score, value, ((1,), (0,)))
            reach = near * jnp.exp(middle)
            if at > 0:
                result = result + spread_dot(
                    reach.astype(jnp.bfloat16), state.astype(jnp.bfloat16), ((1,), (1,))
                )
            loc_ref[rows, there] = result
            qt_ref[rows, here] = (reach * jnp.exp(before)).astype(jnp.bfloat16)
            kept = (rise * jnp.exp(last - middle)).astype(jnp.bfloat16)
            state = jnp.exp(last) * state + spread_dot(value, kept, ((0,), (0,)))
            before = before + last
        for j in range(count):
            parts_ref[j, head, 0:part, :] = state[j * part : (j + 1) * part, :].astype(
                jnp.bfloat16
            )
        tot_ref[pl.ds(head, 1), :] = before
        return carry

    lax.fori_loop(0, heads, one_head, 0)
    total = tot_ref[...]
    top = total.astype(jnp.bfloat16).astype(jnp.float32)
    deep = parts_ref.shape[2]
    filler = [jnp.zeros((deep - 2 * heads, width), jnp.float32)] if deep > 2 * heads else []
    logs = jnp.concatenate([top, total - top] + filler, axis=0).astype(jnp.bfloat16)
    for j in range(count):
        parts_ref[j, heads] = logs

    pl.semaphore_wait(barrier, count + mates - 2)

    def exchange(source, target, send_sem, recv_sem):
        copies = []
        for d in range(1, count):
            peer = lax.rem(me + d, count)
            copy = pltpu.make_async_remote_copy(
                src_ref=source.at[peer], dst_ref=target.at[me],
                send_sem=send_sem.at[d], recv_sem=recv_sem.at[d],
                device_id={"sp": peer}, device_id_type=pl.DeviceIdType.MESH,
            )
            copy.start()
            copies.append(copy)
        target[me] = source[me]
        for copy in copies:
            copy.wait_recv()
        return copies

    first = exchange(parts_ref, came_ref, ready_sem, came_sem)
    so_far = [jnp.zeros((part, width), jnp.float32) for _ in range(heads)]
    for i in range(count):
        marks = came_ref[i, heads].astype(jnp.float32)
        fade = jnp.exp(marks[0:heads, :] + marks[heads : 2 * heads, :])
        for h in range(heads):
            answer_ref[i, h] = so_far[h].astype(jnp.bfloat16)
            piece = came_ref[i, h].astype(jnp.float32)[0:part, :]
            so_far[h] = fade[h : h + 1, :] * so_far[h] + piece
    second = exchange(answer_ref, back_ref, answer_sem, back_sem)
    for i in range(count):
        for h in range(heads):
            prior_ref[h, i * part : (i + 1) * part, :] = back_ref[i, h].astype(jnp.float32)

    own_rows = length // mates
    wide = heads * vwidth
    third = []
    mine_at = pl.ds(pl.multiple_of(lane * wide, wide), wide)
    for d in range(1, mates + 1):
        peer = lax.rem(lane + d, mates)
        rows = pl.ds(pl.multiple_of(peer * own_rows, own_rows), own_rows)
        pieces = []
        for h in range(heads):
            there = slice(h * vwidth, (h + 1) * vwidth)
            full = loc_ref[rows, there] + spread_dot(
                qt_ref[rows, h * width : (h + 1) * width],
                prior_ref[h].astype(jnp.bfloat16), ((1,), (1,)),
            )
            square = jnp.mean(full * full, axis=1, keepdims=True)
            gate = g_ref[rows, there].astype(jnp.float32)
            scaled = full * lax.rsqrt(square + 1e-06) * n_ref[:, there]
            pieces.append((scaled * (gate * jax.nn.sigmoid(gate))).astype(jnp.bfloat16))
        gated = jnp.concatenate(pieces, axis=1)
        if d == mates:
            out_ref[:, mine_at] = gated
        else:
            rows_ref[d - 1] = gated
            copy = pltpu.make_async_remote_copy(
                src_ref=rows_ref.at[d - 1], dst_ref=out_ref.at[:, mine_at],
                send_sem=rows_sem.at[d], recv_sem=out_sem.at[d],
                device_id={"tp": peer}, device_id_type=pl.DeviceIdType.MESH,
            )
            copy.start()
            third.append(copy)
    for copy in third:
        copy.wait_recv()
    fetch.wait()
    model = matrix_ref.shape[1]
    tile = model // 4
    for at in range(4):
        cols = slice(at * tile, (at + 1) * tile)
        mixed = jnp.dot(
            out_ref[...], matrix_ref[:, cols], preferred_element_type=jnp.float32
        )
        stream_ref[:, cols] = (r_ref[:, cols].astype(jnp.float32) + mixed).astype(jnp.bfloat16)
    for copy in first + second + third:
        copy.wait_send()


def gated_arrivals(query, forget_logits, margin, spike, value_logits, gate_logits, head_scale, matrix, resid):
    length, columns = query.shape
    heads = spike.shape[1]
    width = columns // heads
    wide = value_logits.shape[1]
    vwidth = wide // heads
    count, mates = lax.axis_size("sp"), lax.axis_size("tp")
    part = vwidth // count
    deep = max(part, 2 * heads)
    rows = length // mates
    vmem = pl.BlockSpec(memory_space=pltpu.VMEM)
    return pl.pallas_call(
        mixing_kernel,
        in_specs=[vmem] * 7 + [pl.BlockSpec(memory_space=pl.ANY), vmem],
        out_specs=vmem,
        out_shape=jax.ShapeDtypeStruct(resid.shape, jnp.bfloat16),
        scratch_shapes=[
            pltpu.VMEM((length, wide), jnp.float32),
            pltpu.VMEM((length, columns), jnp.bfloat16),
            pltpu.VMEM((heads, width), jnp.float32),
            pltpu.VMEM((count, heads + 1, deep, width), jnp.bfloat16),
            pltpu.VMEM((count, heads + 1, deep, width), jnp.bfloat16),
            pltpu.VMEM((count, heads, part, width), jnp.bfloat16),
            pltpu.VMEM((count, heads, part, width), jnp.bfloat16),
            pltpu.VMEM((heads, vwidth, width), jnp.float32),
            pltpu.VMEM((mates - 1, rows, wide), jnp.bfloat16),
            pltpu.VMEM((rows, mates * wide), jnp.bfloat16),
            pltpu.VMEM(matrix.shape, matrix.dtype),
            pltpu.SemaphoreType.DMA((count,)),
            pltpu.SemaphoreType.DMA((count,)),
            pltpu.SemaphoreType.DMA((count,)),
            pltpu.SemaphoreType.DMA((count,)),
            pltpu.SemaphoreType.DMA((mates,)),
            pltpu.SemaphoreType.DMA((mates,)),
            pltpu.SemaphoreType.DMA,
        ],
        compiler_params=pltpu.CompilerParams(collective_id=0, has_side_effects=True),
    )(
        query, forget_logits, margin[None, :], spike.T, value_logits, gate_logits,
        head_scale[None, :], matrix, resid,
    )


CHUNKS = 2
TILE = 256
SLOTS = 16


def tile_of(extent):
    return min(TILE, extent)


def expert_kernel(
    stream_ref, scale_ref, routes_ref, weight_ref, gate_ref, up_ref, down_ref, out_ref,
    normed_ref, meta_ref, pack_ref, came_ref, hidden_ref, answer_ref, back_ref, part_ref, far_ref, total_ref,
    gate_vmem, up_vmem, down_vmem,
    load_sem, meta_send, meta_recv, over_send, over_recv, out_send, out_recv,
    ret_send, ret_recv, home_send, home_recv,
):
    rows, model = stream_ref.shape
    hidden = gate_vmem.shape[1]
    count, mates = lax.axis_size("sp"), lax.axis_size("tp")
    me, lane = lax.axis_index("sp"), lax.axis_index("tp")
    near = count // 2
    side = me // near
    peers = near * mates
    spot = (me - side * near) * mates + lane
    mirror = lax.rem(me + near, count)
    slots = came_ref.shape[1] // peers
    experts = peers * 2
    wide = model // CHUNKS

    loads = []
    for at, (source, target) in enumerate(
        ((gate_ref, gate_vmem), (up_ref, up_vmem), (down_ref, down_vmem))
    ):
        copy = pltpu.make_async_copy(source.at[0], target, load_sem.at[at])
        copy.start()
        loads.append(copy)

    def place(d):
        other = lax.rem(spot + d, peers)
        return other, {"sp": side * near + other // mates, "tp": lax.rem(other, mates)}

    barrier = pltpu.get_barrier_semaphore()
    pl.semaphore_signal(
        barrier, inc=1, device_id={"sp": mirror}, device_id_type=pl.DeviceIdType.MESH
    )

    def greet(d, carry):
        pl.semaphore_signal(
            barrier, inc=1, device_id=place(d)[1], device_id_type=pl.DeviceIdType.MESH
        )
        return carry

    lax.fori_loop(1, peers, greet, 0)

    values = stream_ref[...].astype(jnp.float32)
    square = jnp.mean(values * values, axis=1, keepdims=True)
    normed_ref[0] = (values * lax.rsqrt(square + 1e-06) * scale_ref[...]).astype(jnp.bfloat16)

    routes = routes_ref[...]
    named = lax.broadcasted_iota(jnp.int32, (experts, rows), 0)
    hits = [named == routes[k : k + 1, :] for k in range(2)]
    member = (hits[0] | hits[1]).astype(jnp.float32).astype(jnp.bfloat16)
    earlier = (
        lax.broadcasted_iota(jnp.int32, (rows, rows), 0)
        < lax.broadcasted_iota(jnp.int32, (rows, rows), 1)
    ).astype(jnp.float32).astype(jnp.bfloat16)
    ranks = spread_dot(member, earlier, ((1,), (0,)))
    for k in range(2):
        rank = jnp.sum(jnp.where(hits[k], ranks, 0.0), axis=0, keepdims=True)
        meta_ref[0, k : k + 1, :] = routes[k : k + 1, :].astype(jnp.float32) * slots + rank
        meta_ref[0, 2 + k : 3 + k, :] = weight_ref[k : k + 1, :]
    meta_ref[0, 4:8, :] = jnp.zeros((4, rows), jnp.float32)

    pl.semaphore_wait(barrier, peers)

    def across(source, target, send_sem, recv_sem):
        return pltpu.make_async_remote_copy(
            src_ref=source, dst_ref=target, send_sem=send_sem, recv_sem=recv_sem,
            device_id={"sp": mirror}, device_id_type=pl.DeviceIdType.MESH,
        )

    note = across(meta_ref.at[0], meta_ref.at[1], meta_send, meta_recv)
    note.start()
    over = []
    for c in range(CHUNKS):
        cols = pl.ds(c * wide, wide)
        copy = across(
            normed_ref.at[0, :, cols], normed_ref.at[1, :, cols], over_send.at[c], over_recv.at[c]
        )
        copy.start()
        over.append(copy)

    def mine_at():
        return pl.ds(pl.multiple_of(spot * slots, slots), slots)

    def parcel(source, target, block, cols, turn, d, send_sem, recv_sem):
        other, device = place(d)
        there = pl.ds(pl.multiple_of(other * slots, slots), slots)
        return pltpu.make_async_remote_copy(
            src_ref=source.at[block, there, cols], dst_ref=target.at[block, mine_at(), cols],
            send_sem=send_sem.at[turn, d], recv_sem=recv_sem.at[turn, d],
            device_id=device, device_id_type=pl.DeviceIdType.MESH,
        )

    def spread(source, target, block, cols, turn, send_sem, recv_sem):
        def step(d, carry):
            parcel(source, target, block, cols, turn, d, send_sem, recv_sem).start()
            return carry

        lax.fori_loop(1, peers, step, 0)
        target[block, mine_at(), cols] = source[block, mine_at(), cols]

    def arrive(source, target, block, cols, turn, send_sem, recv_sem):
        def step(d, carry):
            parcel(source, target, block, cols, turn, d, send_sem, recv_sem).wait_recv()
            return carry

        lax.fori_loop(1, peers, step, 0)

    def depart(source, target, block, cols, turn, send_sem, recv_sem):
        def step(d, carry):
            parcel(source, target, block, cols, turn, d, send_sem, recv_sem).wait_send()
            return carry

        lax.fori_loop(1, peers, step, 0)

    lot = lax.broadcasted_iota(jnp.int32, (peers * slots, rows), 0).astype(jnp.float32)

    def picks(block):
        first = (side * peers * slots).astype(jnp.float32)
        return [lot == meta_ref[block, k : k + 1, :] - first for k in range(2)]

    def pack(block, cols):
        chosen = picks(block)
        select = (chosen[0] | chosen[1]).astype(jnp.float32).astype(jnp.bfloat16)
        extent = cols.size
        step = tile_of(extent)
        for at in range(extent // step):
            here = pl.ds(cols.start + at * step, step)
            pack_ref[block, :, here] = spread_dot(
                select, normed_ref[block, :, here], ((1,), (0,))
            ).astype(jnp.bfloat16)

    def enter(block):
        def step(at, carry):
            here = pl.ds(pl.multiple_of(at * tile_of(hidden), tile_of(hidden)), tile_of(hidden))
            gate = spread_dot(came_ref[block], gate_vmem[:, here], ((1,), (0,)))
            up = spread_dot(came_ref[block], up_vmem[:, here], ((1,), (0,)))
            hidden_ref[:, here] = (gate * jax.nn.sigmoid(gate) * up).astype(jnp.bfloat16)
            return carry

        lax.fori_loop(0, hidden // tile_of(hidden), step, 0)

    def leave(block, cols):
        size = tile_of(cols.size)

        def step(at, carry):
            here = pl.ds(pl.multiple_of(cols.start + at * size, size), size)
            answer_ref[block, :, here] = spread_dot(
                hidden_ref[...], down_vmem[:, here], ((1,), (0,))
            ).astype(jnp.bfloat16)
            return carry

        lax.fori_loop(0, cols.size // size, step, 0)

    def weights(block):
        chosen = picks(block)
        load = jnp.where(chosen[0], meta_ref[block, 2:3, :], 0.0) + jnp.where(
            chosen[1], meta_ref[block, 3:4, :], 0.0
        )
        high = load.astype(jnp.bfloat16)
        return high, (load - high.astype(jnp.float32)).astype(jnp.bfloat16)

    def gather(block, here, high, low):
        piece = back_ref[block, :, here]
        return spread_dot(high, piece, ((0,), (0,))) + spread_dot(low, piece, ((0,), (0,)))

    whole = pl.ds(0, model)
    parts = [pl.ds(c * wide, wide) for c in range(CHUNKS)]

    pack(0, whole)
    spread(pack_ref, came_ref, 0, whole, 0, out_send, out_recv)
    for copy in loads:
        copy.wait()
    arrive(pack_ref, came_ref, 0, whole, 0, out_send, out_recv)
    enter(0)
    leave(0, whole)
    spread(answer_ref, back_ref, 0, whole, 0, ret_send, ret_recv)

    note.wait_recv()
    for c in range(CHUNKS):
        over[c].wait_recv()
        pack(1, parts[c])
        spread(pack_ref, came_ref, 1, parts[c], 1 + c, out_send, out_recv)
    for c in range(CHUNKS):
        arrive(pack_ref, came_ref, 1, parts[c], 1 + c, out_send, out_recv)
    enter(1)
    for c in range(CHUNKS):
        leave(1, parts[c])
        spread(answer_ref, back_ref, 1, parts[c], 1 + c, ret_send, ret_recv)

    home = []
    high, low = weights(1)
    for c in range(CHUNKS):
        arrive(answer_ref, back_ref, 1, parts[c], 1 + c, ret_send, ret_recv)
        size = tile_of(wide)
        for at in range(wide // size):
            here = pl.ds(c * wide + at * size, size)
            part_ref[:, here] = gather(1, here, high, low).astype(jnp.bfloat16)
        copy = across(
            part_ref.at[:, parts[c]], far_ref.at[:, parts[c]], home_send.at[c], home_recv.at[c]
        )
        copy.start()
        home.append(copy)

    arrive(answer_ref, back_ref, 0, whole, 0, ret_send, ret_recv)
    high, low = weights(0)
    for at in range(model // tile_of(model)):
        here = pl.ds(at * tile_of(model), tile_of(model))
        total_ref[:, here] = stream_ref[:, here].astype(jnp.float32) + gather(0, here, high, low)
    for c in range(CHUNKS):
        home[c].wait_recv()
        out_ref[:, parts[c]] = (
            total_ref[:, parts[c]] + far_ref[:, parts[c]].astype(jnp.float32)
        ).astype(jnp.bfloat16)

    note.wait_send()
    for copy in over + home:
        copy.wait_send()
    depart(pack_ref, came_ref, 0, whole, 0, out_send, out_recv)
    depart(answer_ref, back_ref, 0, whole, 0, ret_send, ret_recv)
    for c in range(CHUNKS):
        depart(pack_ref, came_ref, 1, parts[c], 1 + c, out_send, out_recv)
        depart(answer_ref, back_ref, 1, parts[c], 1 + c, ret_send, ret_recv)


def routed_experts(stream, scale, routes, weight, gate_matrix, up_matrix, down_matrix):
    rows, model = stream.shape
    hidden = gate_matrix.shape[2]
    peers = lax.axis_size("sp") // 2 * lax.axis_size("tp")
    capacity = 2 * rows * routes.shape[1] // (2 * peers * gate_matrix.shape[0])
    slots = -(-capacity // SLOTS) * SLOTS
    vmem = pl.BlockSpec(memory_space=pltpu.VMEM)
    anywhere = pl.BlockSpec(memory_space=pl.ANY)
    blocks = pltpu.VMEM((2, peers * slots, model), jnp.bfloat16)
    pair = pltpu.SemaphoreType.DMA((CHUNKS,))
    fan = pltpu.SemaphoreType.DMA((1 + CHUNKS, peers))
    return pl.pallas_call(
        expert_kernel,
        in_specs=[vmem] * 4 + [anywhere] * 3,
        out_specs=vmem,
        out_shape=jax.ShapeDtypeStruct((rows, model), jnp.bfloat16),
        scratch_shapes=[
            pltpu.VMEM((2, rows, model), jnp.bfloat16),
            pltpu.VMEM((2, 8, rows), jnp.float32),
            blocks,
            blocks,
            pltpu.VMEM((peers * slots, hidden), jnp.bfloat16),
            blocks,
            blocks,
            pltpu.VMEM((rows, model), jnp.bfloat16),
            pltpu.VMEM((rows, model), jnp.bfloat16),
            pltpu.VMEM((rows, model), jnp.float32),
            pltpu.VMEM((model, hidden), jnp.bfloat16),
            pltpu.VMEM((model, hidden), jnp.bfloat16),
            pltpu.VMEM((hidden, model), jnp.bfloat16),
            pltpu.SemaphoreType.DMA((3,)),
            pltpu.SemaphoreType.DMA,
            pltpu.SemaphoreType.DMA,
            pair, pair, fan, fan, fan, fan, pair, pair,
        ],
        compiler_params=pltpu.CompilerParams(collective_id=1, has_side_effects=True),
    )(stream, scale[None, :], routes.T, weight.T, gate_matrix, up_matrix, down_matrix)


def body(
    resid,
    query,
    forget_logits,
    forget_margin,
    decay_spike,
    value_logits,
    output_gate_logits,
    head_norm_scale,
    output_matrix,
    norm_scale_vector,
    routes,
    routing_weight,
    gate_matrix,
    up_matrix,
    down_matrix,
):
    stream = gated_arrivals(
        query, forget_logits, forget_margin, decay_spike, value_logits,
        output_gate_logits, head_norm_scale, output_matrix, resid,
    )
    return routed_experts(
        stream, norm_scale_vector, routes, routing_weight, gate_matrix, up_matrix, down_matrix
    )


def solution(mesh):
    return jax.shard_map(
        body,
        mesh=mesh,
        in_specs=(
            P(("sp", "tp"), None),
            P("sp", "tp"),
            P("sp", "tp"),
            P("tp"),
            P("sp", "tp"),
            P("sp", "tp"),
            P("sp", "tp"),
            P("tp"),
            P(),
            P(),
            P(("sp", "tp"), None),
            P(("sp", "tp"), None),
            P(("sp", "tp"), None, None),
            P(("sp", "tp"), None, None),
            P(("sp", "tp"), None, None),
        ),
        out_specs=P(("sp", "tp"), None),
        check_vma=False,
    )
```

```python
import jax
import jax.numpy as jnp
from jax import lax
from jax.experimental import pallas as pl
from jax.experimental.pallas import tpu as pltpu
from jax.sharding import PartitionSpec as P

DK = 128
BLOCK = 64


SPAN = 2 * BLOCK


def spread_dot(left, right, dims):
    return lax.dot_general(left, right, (dims, ((), ())), preferred_element_type=jnp.float32)


def mixing_kernel(
    q_ref, f_ref, m_ref, s_ref, v_ref, g_ref, n_ref, w_ref, r_ref, stream_ref,
    loc_ref, qt_ref, tot_ref, parts_ref, came_ref, answer_ref, back_ref, prior_ref, rows_ref,
    out_ref, matrix_ref,
    ready_sem, came_sem, answer_sem, back_sem, rows_sem, out_sem, matrix_sem,
):
    length, columns = q_ref.shape
    heads = s_ref.shape[0]
    width = columns // heads
    vwidth = v_ref.shape[1] // heads
    count, mates = lax.axis_size("sp"), lax.axis_size("tp")
    me, lane = lax.axis_index("sp"), lax.axis_index("tp")
    part = vwidth // count
    barrier = pltpu.get_barrier_semaphore()
    fetch = pltpu.make_async_copy(w_ref, matrix_ref, matrix_sem)
    fetch.start()
    for d in range(1, count):
        pl.semaphore_signal(
            barrier, inc=1, device_id={"sp": lax.rem(me + d, count)},
            device_id_type=pl.DeviceIdType.MESH,
        )
    for d in range(1, mates):
        pl.semaphore_signal(
            barrier, inc=1, device_id={"tp": lax.rem(lane + d, mates)},
            device_id_type=pl.DeviceIdType.MESH,
        )

    span = min(SPAN, length)
    lower = lax.broadcasted_iota(jnp.int32, (span, span), 0) >= lax.broadcasted_iota(
        jnp.int32, (span, span), 1
    )
    ones = lower.astype(jnp.float32).astype(jnp.bfloat16)
    spot = lax.broadcasted_iota(jnp.int32, (2 * heads, width), 0)

    def one_head(head, carry):
        here = pl.ds(pl.multiple_of(head * width, width), width)
        there = pl.ds(pl.multiple_of(head * vwidth, vwidth), vwidth)
        mine = ((spot == head) | (spot == head + heads)).astype(jnp.float32).astype(jnp.bfloat16)
        margin = m_ref[:, here]
        state = jnp.zeros((vwidth, width), jnp.float32)
        before = jnp.zeros((1, width), jnp.float32)
        for at in range(length // span):
            rows = pl.ds(at * span, span)
            keys = margin * jax.nn.sigmoid(-f_ref[rows, here].astype(jnp.float32))
            spikes = s_ref[:, rows]
            top = spikes.astype(jnp.bfloat16).astype(jnp.float32)
            halves = jnp.concatenate([top, spikes - top], axis=0).astype(jnp.bfloat16)
            decay = jnp.log1p(-keys) + spread_dot(halves, mine, ((0,), (0,)))
            high = decay.astype(jnp.bfloat16)
            low = (decay - high.astype(jnp.float32)).astype(jnp.bfloat16)
            both = spread_dot(ones, jnp.concatenate([high, low], axis=1), ((1,), (0,)))
            cum = both[:, :width] + both[:, width:]
            middle = cum[span // 2 - 1 : span // 2, :]
            last = cum[span - 1 : span, :]
            down = jnp.exp(cum - middle)
            up = jnp.exp(middle - cum)
            query = q_ref[rows, here].astype(jnp.float32) * DK ** (-0.5)
            logits = v_ref[rows, there].astype(jnp.float32)
            value = (logits * jax.nn.sigmoid(logits)).astype(jnp.bfloat16)
            near = query * down
            rise = keys * up
            score = spread_dot(
                near.astype(jnp.bfloat16), rise.astype(jnp.bfloat16), ((1,), (1,))
            )
            score = jnp.where(lower, score, 0.0).astype(jnp.bfloat16)
            result = spread_dot(score, value, ((1,), (0,)))
            reach = near * jnp.exp(middle)
            if at > 0:
                result = result + spread_dot(
                    reach.astype(jnp.bfloat16), state.astype(jnp.bfloat16), ((1,), (1,))
                )
            loc_ref[rows, there] = result
            qt_ref[rows, here] = (reach * jnp.exp(before)).astype(jnp.bfloat16)
            kept = (rise * jnp.exp(last - middle)).astype(jnp.bfloat16)
            state = jnp.exp(last) * state + spread_dot(value, kept, ((0,), (0,)))
            before = before + last
        for j in range(count):
            parts_ref[j, head, 0:part, :] = state[j * part : (j + 1) * part, :].astype(
                jnp.bfloat16
            )
        tot_ref[pl.ds(head, 1), :] = before
        return carry

    lax.fori_loop(0, heads, one_head, 0)
    total = tot_ref[...]
    top = total.astype(jnp.bfloat16).astype(jnp.float32)
    deep = parts_ref.shape[2]
    filler = [jnp.zeros((deep - 2 * heads, width), jnp.float32)] if deep > 2 * heads else []
    logs = jnp.concatenate([top, total - top] + filler, axis=0).astype(jnp.bfloat16)
    for j in range(count):
        parts_ref[j, heads] = logs

    pl.semaphore_wait(barrier, count + mates - 2)

    def exchange(source, target, send_sem, recv_sem):
        copies = []
        for d in range(1, count):
            peer = lax.rem(me + d, count)
            copy = pltpu.make_async_remote_copy(
                src_ref=source.at[peer], dst_ref=target.at[me],
                send_sem=send_sem.at[d], recv_sem=recv_sem.at[d],
                device_id={"sp": peer}, device_id_type=pl.DeviceIdType.MESH,
            )
            copy.start()
            copies.append(copy)
        target[me] = source[me]
        for copy in copies:
            copy.wait_recv()
        return copies

    first = exchange(parts_ref, came_ref, ready_sem, came_sem)
    so_far = [jnp.zeros((part, width), jnp.float32) for _ in range(heads)]
    for i in range(count):
        marks = came_ref[i, heads].astype(jnp.float32)
        fade = jnp.exp(marks[0:heads, :] + marks[heads : 2 * heads, :])
        for h in range(heads):
            answer_ref[i, h] = so_far[h].astype(jnp.bfloat16)
            piece = came_ref[i, h].astype(jnp.float32)[0:part, :]
            so_far[h] = fade[h : h + 1, :] * so_far[h] + piece
    second = exchange(answer_ref, back_ref, answer_sem, back_sem)
    for i in range(count):
        for h in range(heads):
            prior_ref[h, i * part : (i + 1) * part, :] = back_ref[i, h].astype(jnp.float32)

    own_rows = length // mates
    wide = heads * vwidth
    third = []
    mine_at = pl.ds(pl.multiple_of(lane * wide, wide), wide)
    for d in range(1, mates + 1):
        peer = lax.rem(lane + d, mates)
        rows = pl.ds(pl.multiple_of(peer * own_rows, own_rows), own_rows)
        pieces = []
        for h in range(heads):
            there = slice(h * vwidth, (h + 1) * vwidth)
            full = loc_ref[rows, there] + spread_dot(
                qt_ref[rows, h * width : (h + 1) * width],
                prior_ref[h].astype(jnp.bfloat16), ((1,), (1,)),
            )
            square = jnp.mean(full * full, axis=1, keepdims=True)
            gate = g_ref[rows, there].astype(jnp.float32)
            scaled = full * lax.rsqrt(square + 1e-06) * n_ref[:, there]
            pieces.append((scaled * (gate * jax.nn.sigmoid(gate))).astype(jnp.bfloat16))
        gated = jnp.concatenate(pieces, axis=1)
        if d == mates:
            out_ref[:, mine_at] = gated
        else:
            rows_ref[d - 1] = gated
            copy = pltpu.make_async_remote_copy(
                src_ref=rows_ref.at[d - 1], dst_ref=out_ref.at[:, mine_at],
                send_sem=rows_sem.at[d], recv_sem=out_sem.at[d],
                device_id={"tp": peer}, device_id_type=pl.DeviceIdType.MESH,
            )
            copy.start()
            third.append(copy)
    for copy in third:
        copy.wait_recv()
    fetch.wait()
    model = matrix_ref.shape[1]
    tile = model // 4
    for at in range(4):
        cols = slice(at * tile, (at + 1) * tile)
        mixed = jnp.dot(
            out_ref[...], matrix_ref[:, cols], preferred_element_type=jnp.float32
        )
        stream_ref[:, cols] = (r_ref[:, cols].astype(jnp.float32) + mixed).astype(jnp.bfloat16)
    for copy in first + second + third:
        copy.wait_send()


def gated_arrivals(query, forget_logits, margin, spike, value_logits, gate_logits, head_scale, matrix, resid):
    length, columns = query.shape
    heads = spike.shape[1]
    width = columns // heads
    wide = value_logits.shape[1]
    vwidth = wide // heads
    count, mates = lax.axis_size("sp"), lax.axis_size("tp")
    part = vwidth // count
    deep = max(part, 2 * heads)
    rows = length // mates
    vmem = pl.BlockSpec(memory_space=pltpu.VMEM)
    return pl.pallas_call(
        mixing_kernel,
        in_specs=[vmem] * 7 + [pl.BlockSpec(memory_space=pl.ANY), vmem],
        out_specs=vmem,
        out_shape=jax.ShapeDtypeStruct(resid.shape, jnp.bfloat16),
        scratch_shapes=[
            pltpu.VMEM((length, wide), jnp.float32),
            pltpu.VMEM((length, columns), jnp.bfloat16),
            pltpu.VMEM((heads, width), jnp.float32),
            pltpu.VMEM((count, heads + 1, deep, width), jnp.bfloat16),
            pltpu.VMEM((count, heads + 1, deep, width), jnp.bfloat16),
            pltpu.VMEM((count, heads, part, width), jnp.bfloat16),
            pltpu.VMEM((count, heads, part, width), jnp.bfloat16),
            pltpu.VMEM((heads, vwidth, width), jnp.float32),
            pltpu.VMEM((mates - 1, rows, wide), jnp.bfloat16),
            pltpu.VMEM((rows, mates * wide), jnp.bfloat16),
            pltpu.VMEM(matrix.shape, matrix.dtype),
            pltpu.SemaphoreType.DMA((count,)),
            pltpu.SemaphoreType.DMA((count,)),
            pltpu.SemaphoreType.DMA((count,)),
            pltpu.SemaphoreType.DMA((count,)),
            pltpu.SemaphoreType.DMA((mates,)),
            pltpu.SemaphoreType.DMA((mates,)),
            pltpu.SemaphoreType.DMA,
        ],
        compiler_params=pltpu.CompilerParams(collective_id=0, has_side_effects=True),
    )(
        query, forget_logits, margin[None, :], spike.T, value_logits, gate_logits,
        head_scale[None, :], matrix, resid,
    )


CHUNKS = 2
TILE = 256
SLOTS = 16


def tile_of(extent):
    return min(TILE, extent)


def expert_kernel(
    stream_ref, scale_ref, routes_ref, weight_ref, gate_ref, up_ref, down_ref, out_ref,
    normed_ref, meta_ref, pack_ref, came_ref, hidden_ref, answer_ref, back_ref, part_ref, far_ref, total_ref,
    gate_vmem, up_vmem, down_vmem,
    load_sem, meta_send, meta_recv, over_send, over_recv, out_send, out_recv,
    ret_send, ret_recv, home_send, home_recv,
):
    rows, model = stream_ref.shape
    hidden = gate_vmem.shape[1]
    count, mates = lax.axis_size("sp"), lax.axis_size("tp")
    me, lane = lax.axis_index("sp"), lax.axis_index("tp")
    near = count // 2
    side = me // near
    peers = near * mates
    spot = (me - side * near) * mates + lane
    mirror = lax.rem(me + near, count)
    slots = came_ref.shape[1] // peers
    experts = peers * 2
    wide = model // CHUNKS

    loads = []
    for at, (source, target) in enumerate(
        ((gate_ref, gate_vmem), (up_ref, up_vmem), (down_ref, down_vmem))
    ):
        copy = pltpu.make_async_copy(source.at[0], target, load_sem.at[at])
        copy.start()
        loads.append(copy)

    bits = [1 << k for k in range(peers.bit_length() - 1)]
    assert 1 << len(bits) == peers
    flips = [(1 - 2 * lax.rem(spot // bit, 2)) * bit for bit in bits]

    def place(d):
        mask = d
        other = spot + sum(lax.rem(mask // bit, 2) * flip for bit, flip in zip(bits, flips))
        return other, {"sp": side * near + other // mates, "tp": lax.rem(other, mates)}

    barrier = pltpu.get_barrier_semaphore()
    pl.semaphore_signal(
        barrier, inc=1, device_id={"sp": mirror}, device_id_type=pl.DeviceIdType.MESH
    )

    def greet(d, carry):
        pl.semaphore_signal(
            barrier, inc=1, device_id=place(d)[1], device_id_type=pl.DeviceIdType.MESH
        )
        return carry

    lax.fori_loop(1, peers, greet, 0)

    values = stream_ref[...].astype(jnp.float32)
    square = jnp.mean(values * values, axis=1, keepdims=True)
    normed_ref[0] = (values * lax.rsqrt(square + 1e-06) * scale_ref[...]).astype(jnp.bfloat16)

    routes = routes_ref[...]
    named = lax.broadcasted_iota(jnp.int32, (experts, rows), 0)
    hits = [named == routes[k : k + 1, :] for k in range(2)]
    member = (hits[0] | hits[1]).astype(jnp.float32).astype(jnp.bfloat16)
    earlier = (
        lax.broadcasted_iota(jnp.int32, (rows, rows), 0)
        < lax.broadcasted_iota(jnp.int32, (rows, rows), 1)
    ).astype(jnp.float32).astype(jnp.bfloat16)
    ranks = spread_dot(member, earlier, ((1,), (0,)))
    for k in range(2):
        rank = jnp.sum(jnp.where(hits[k], ranks, 0.0), axis=0, keepdims=True)
        meta_ref[0, k : k + 1, :] = routes[k : k + 1, :].astype(jnp.float32) * slots + rank
        meta_ref[0, 2 + k : 3 + k, :] = weight_ref[k : k + 1, :]
    meta_ref[0, 4:8, :] = jnp.zeros((4, rows), jnp.float32)

    pl.semaphore_wait(barrier, peers)

    def across(source, target, send_sem, recv_sem):
        return pltpu.make_async_remote_copy(
            src_ref=source, dst_ref=target, send_sem=send_sem, recv_sem=recv_sem,
            device_id={"sp": mirror}, device_id_type=pl.DeviceIdType.MESH,
        )

    note = across(meta_ref.at[0], meta_ref.at[1], meta_send, meta_recv)
    note.start()
    over = []
    for c in range(CHUNKS):
        cols = pl.ds(c * wide, wide)
        copy = across(
            normed_ref.at[0, :, cols], normed_ref.at[1, :, cols], over_send.at[c], over_recv.at[c]
        )
        copy.start()
        over.append(copy)

    def mine_at():
        return pl.ds(pl.multiple_of(spot * slots, slots), slots)

    def parcel(source, target, block, cols, turn, d, send_sem, recv_sem):
        other, device = place(d)
        there = pl.ds(pl.multiple_of(other * slots, slots), slots)
        return pltpu.make_async_remote_copy(
            src_ref=source.at[block, there, cols], dst_ref=target.at[block, mine_at(), cols],
            send_sem=send_sem.at[turn, d], recv_sem=recv_sem.at[turn, d],
            device_id=device, device_id_type=pl.DeviceIdType.MESH,
        )

    def spread(source, target, block, cols, turn, send_sem, recv_sem):
        def step(d, carry):
            parcel(source, target, block, cols, turn, d, send_sem, recv_sem).start()
            return carry

        lax.fori_loop(1, peers, step, 0)
        target[block, mine_at(), cols] = source[block, mine_at(), cols]

    def arrive(source, target, block, cols, turn, send_sem, recv_sem):
        def step(d, carry):
            parcel(source, target, block, cols, turn, d, send_sem, recv_sem).wait_recv()
            return carry

        lax.fori_loop(1, peers, step, 0)

    def depart(source, target, block, cols, turn, send_sem, recv_sem):
        def step(d, carry):
            parcel(source, target, block, cols, turn, d, send_sem, recv_sem).wait_send()
            return carry

        lax.fori_loop(1, peers, step, 0)

    lot = lax.broadcasted_iota(jnp.int32, (peers * slots, rows), 0).astype(jnp.float32)

    def picks(block):
        first = (side * peers * slots).astype(jnp.float32)
        return [lot == meta_ref[block, k : k + 1, :] - first for k in range(2)]

    def pack(block, cols):
        chosen = picks(block)
        select = (chosen[0] | chosen[1]).astype(jnp.float32).astype(jnp.bfloat16)
        extent = cols.size
        step = tile_of(extent)
        for at in range(extent // step):
            here = pl.ds(cols.start + at * step, step)
            pack_ref[block, :, here] = spread_dot(
                select, normed_ref[block, :, here], ((1,), (0,))
            ).astype(jnp.bfloat16)

    def enter(block):
        def step(at, carry):
            here = pl.ds(pl.multiple_of(at * tile_of(hidden), tile_of(hidden)), tile_of(hidden))
            gate = spread_dot(came_ref[block], gate_vmem[:, here], ((1,), (0,)))
            up = spread_dot(came_ref[block], up_vmem[:, here], ((1,), (0,)))
            hidden_ref[:, here] = (gate * jax.nn.sigmoid(gate) * up).astype(jnp.bfloat16)
            return carry

        lax.fori_loop(0, hidden // tile_of(hidden), step, 0)

    def leave(block, cols):
        size = tile_of(cols.size)

        def step(at, carry):
            here = pl.ds(pl.multiple_of(cols.start + at * size, size), size)
            answer_ref[block, :, here] = spread_dot(
                hidden_ref[...], down_vmem[:, here], ((1,), (0,))
            ).astype(jnp.bfloat16)
            return carry

        lax.fori_loop(0, cols.size // size, step, 0)

    def weights(block):
        chosen = picks(block)
        load = jnp.where(chosen[0], meta_ref[block, 2:3, :], 0.0) + jnp.where(
            chosen[1], meta_ref[block, 3:4, :], 0.0
        )
        high = load.astype(jnp.bfloat16)
        return high, (load - high.astype(jnp.float32)).astype(jnp.bfloat16)

    def gather(block, here, high, low):
        piece = back_ref[block, :, here]
        return spread_dot(high, piece, ((0,), (0,))) + spread_dot(low, piece, ((0,), (0,)))

    whole = pl.ds(0, model)
    parts = [pl.ds(c * wide, wide) for c in range(CHUNKS)]

    pack(0, whole)
    spread(pack_ref, came_ref, 0, whole, 0, out_send, out_recv)

    note.wait_recv()
    for c in range(CHUNKS):
        over[c].wait_recv()
        pack(1, parts[c])
        spread(pack_ref, came_ref, 1, parts[c], 1 + c, out_send, out_recv)
    for copy in loads:
        copy.wait()
    arrive(pack_ref, came_ref, 0, whole, 0, out_send, out_recv)
    enter(0)
    leave(0, whole)
    for c in range(CHUNKS):
        arrive(pack_ref, came_ref, 1, parts[c], 1 + c, out_send, out_recv)
    enter(1)
    for c in range(CHUNKS):
        leave(1, parts[c])
        spread(answer_ref, back_ref, 1, parts[c], 1 + c, ret_send, ret_recv)

    spread(answer_ref, back_ref, 0, whole, 0, ret_send, ret_recv)
    home = []
    high, low = weights(1)
    for c in range(CHUNKS):
        arrive(answer_ref, back_ref, 1, parts[c], 1 + c, ret_send, ret_recv)
        size = tile_of(wide)
        for at in range(wide // size):
            here = pl.ds(c * wide + at * size, size)
            part_ref[:, here] = gather(1, here, high, low).astype(jnp.bfloat16)
        copy = across(
            part_ref.at[:, parts[c]], far_ref.at[:, parts[c]], home_send.at[c], home_recv.at[c]
        )
        copy.start()
        home.append(copy)

    arrive(answer_ref, back_ref, 0, whole, 0, ret_send, ret_recv)
    high, low = weights(0)
    for at in range(model // tile_of(model)):
        here = pl.ds(at * tile_of(model), tile_of(model))
        total_ref[:, here] = stream_ref[:, here].astype(jnp.float32) + gather(0, here, high, low)
    for c in range(CHUNKS):
        home[c].wait_recv()
        out_ref[:, parts[c]] = (
            total_ref[:, parts[c]] + far_ref[:, parts[c]].astype(jnp.float32)
        ).astype(jnp.bfloat16)

    note.wait_send()
    for copy in over + home:
        copy.wait_send()
    depart(pack_ref, came_ref, 0, whole, 0, out_send, out_recv)
    depart(answer_ref, back_ref, 0, whole, 0, ret_send, ret_recv)
    for c in range(CHUNKS):
        depart(pack_ref, came_ref, 1, parts[c], 1 + c, out_send, out_recv)
        depart(answer_ref, back_ref, 1, parts[c], 1 + c, ret_send, ret_recv)


def routed_experts(stream, scale, routes, weight, gate_matrix, up_matrix, down_matrix):
    rows, model = stream.shape
    hidden = gate_matrix.shape[2]
    peers = lax.axis_size("sp") // 2 * lax.axis_size("tp")
    capacity = 2 * rows * routes.shape[1] // (2 * peers * gate_matrix.shape[0])
    slots = -(-capacity // SLOTS) * SLOTS
    vmem = pl.BlockSpec(memory_space=pltpu.VMEM)
    anywhere = pl.BlockSpec(memory_space=pl.ANY)
    blocks = pltpu.VMEM((2, peers * slots, model), jnp.bfloat16)
    pair = pltpu.SemaphoreType.DMA((CHUNKS,))
    fan = pltpu.SemaphoreType.DMA((1 + CHUNKS, peers))
    return pl.pallas_call(
        expert_kernel,
        in_specs=[vmem] * 4 + [anywhere] * 3,
        out_specs=vmem,
        out_shape=jax.ShapeDtypeStruct((rows, model), jnp.bfloat16),
        scratch_shapes=[
            pltpu.VMEM((2, rows, model), jnp.bfloat16),
            pltpu.VMEM((2, 8, rows), jnp.float32),
            blocks,
            blocks,
            pltpu.VMEM((peers * slots, hidden), jnp.bfloat16),
            blocks,
            blocks,
            pltpu.VMEM((rows, model), jnp.bfloat16),
            pltpu.VMEM((rows, model), jnp.bfloat16),
            pltpu.VMEM((rows, model), jnp.float32),
            pltpu.VMEM((model, hidden), jnp.bfloat16),
            pltpu.VMEM((model, hidden), jnp.bfloat16),
            pltpu.VMEM((hidden, model), jnp.bfloat16),
            pltpu.SemaphoreType.DMA((3,)),
            pltpu.SemaphoreType.DMA,
            pltpu.SemaphoreType.DMA,
            pair, pair, fan, fan, fan, fan, pair, pair,
        ],
        compiler_params=pltpu.CompilerParams(collective_id=1, has_side_effects=True),
    )(stream, scale[None, :], routes.T, weight.T, gate_matrix, up_matrix, down_matrix)


def body(
    resid,
    query,
    forget_logits,
    forget_margin,
    decay_spike,
    value_logits,
    output_gate_logits,
    head_norm_scale,
    output_matrix,
    norm_scale_vector,
    routes,
    routing_weight,
    gate_matrix,
    up_matrix,
    down_matrix,
):
    stream = gated_arrivals(
        query, forget_logits, forget_margin, decay_spike, value_logits,
        output_gate_logits, head_norm_scale, output_matrix, resid,
    )
    return routed_experts(
        stream, norm_scale_vector, routes, routing_weight, gate_matrix, up_matrix, down_matrix
    )


def solution(mesh):
    return jax.shard_map(
        body,
        mesh=mesh,
        in_specs=(
            P(("sp", "tp"), None),
            P("sp", "tp"),
            P("sp", "tp"),
            P("tp"),
            P("sp", "tp"),
            P("sp", "tp"),
            P("sp", "tp"),
            P("tp"),
            P(),
            P(),
            P(("sp", "tp"), None),
            P(("sp", "tp"), None),
            P(("sp", "tp"), None, None),
            P(("sp", "tp"), None, None),
            P(("sp", "tp"), None, None),
        ),
        out_specs=P(("sp", "tp"), None),
        check_vma=False,
    )
```
